32 devices in a mesh: grp: 2 (over y), ra: 4 (over z), cb: 4 (over x, core).
Axes of the slice: x: 2, y: 2, z: 4, core: 2. Of those that a mesh axis runs over, the one named last changes fastest.
Arguments:
- stream: bfloat16 [256, 4096], P('grp', 'ra'), parts along dimension 0, may hold values from -180 to 180
- w_gate: float32 [2, 4096, 11264], P(None, 'ra', 'cb'), may hold values from -0.09375 to 0.09375
- w_up: float32 [2, 4096, 11264], P(None, 'ra', 'cb'), may hold values from -0.09375 to 0.09375
- w_down: float32 [2, 11264, 4096], P(None, 'cb', 'ra'), may hold values from -0.0546875 to 0.0546875
- gate_scale: float32 [2, 11264], P(None, 'cb'), may hold values from 0.5 to 2
- up_scale: float32 [2, 11264], P(None, 'cb'), may hold values from 0.5 to 2
- down_scale: float32 [2, 4096], P(None, 'ra'), may hold values from 0.5 to 2
- pre_gain: float32 [2, 4096], P(None, 'ra'), may hold values from 0.1 to 1.9
- out_gain: float32 [4096], P('ra'), may hold values from 0.1 to 1.9
Outputs:
- normed: bfloat16 [256, 4096], P('grp', 'ra'), parts along dimension 0
The draws below stay inside these ranges and needn't reach their ends.
There are 2 independent parts, one for each index of `grp`. The reference program is written for one: setup_inputs(seed, part) draws one part's arguments, and reference() takes and returns one part's arrays. A program takes and returns all parts, laid end to end along the dimension named above; an argument that names none is the same for every part. Nothing has to cross between parts.
All inputs are finite; a program needn't handle non-finite values.
Results may differ from the reference program's by a relative error of at most 0.018.
Values may be sent and summed in bfloat16 or wider, within the bound.
A program may use at most 192 MiB of HBM per device.

```python
import math
import jax
import jax.numpy as jnp
from jax import lax

D = 4096
FF = 11264
LAYERS = 2
TOK = 128
N_CB = 4


def draw_stream(key, part):
    first = jax.random.fold_in(key, 11)
    second = jax.random.fold_in(key, 12)
    channel = jnp.exp(math.log(3.0) * jnp.arange(D, dtype=jnp.float32) / D)
    base = jnp.clip(jax.random.normal(first, (TOK, D), jnp.float32), -6.0, 6.0)
    rows = jnp.exp(jax.random.uniform(second, (TOK, 1), jnp.float32, 0.0, math.log(10.0)))
    return (base * rows * channel[None, :]).astype(jnp.bfloat16)


def shard_levels(key, extent, split, least, top_value):
    def one(axis_at, blocks):
        heights = jax.random.uniform(jax.random.fold_in(jax.random.fold_in(key, 6), axis_at), (blocks,), jnp.float32, least / len(split), top_value / len(split))
        return jnp.repeat(jnp.exp(heights), extent[axis_at] // blocks).reshape((-1,) + (1,) * (len(extent) - axis_at - 1))

    factor_of = one(*split[0])
    for cut in split[1:]:
        factor_of = factor_of * one(*cut)
    return factor_of


def gaussian(rng, extent, width, most, cuts=(), held_as=jnp.bfloat16):
    level = shard_levels(rng, extent, cuts, -0.22, 0.18) if cuts else 1.0
    array = jax.random.normal(rng, extent, jnp.float32) * width * level
    return jnp.minimum(jnp.maximum(array, -most), most).astype(held_as)


def setup_inputs(seed: int = 0, part: int = 0) -> dict:
    splits = jax.random.split(jax.random.key(seed), 10)
    part_splits = jax.random.split(jax.random.fold_in(splits[9], part), 10)
    stream = draw_stream(jax.random.fold_in(jax.random.fold_in(splits[9], part), 71), part)
    w_gate = gaussian(splits[1], (LAYERS, D, FF), D ** -0.5, 0.09375, ((1, 4), (2, 4)), jnp.float32)
    w_up = gaussian(splits[2], (LAYERS, D, FF), D ** -0.5, 0.09375, ((1, 4), (2, 4)), jnp.float32)
    w_down = gaussian(splits[3], (LAYERS, FF, D), FF ** -0.5, 0.0546875, ((1, 4), (2, 4)), jnp.float32)
    gate_scale = jnp.clip(jnp.exp(math.log(2.0) - 1.3862944 * jax.random.uniform(splits[4], (LAYERS, FF), jnp.float32) ** shard_levels(splits[4], (LAYERS, FF), ((1, 4),), -0.2, 0.2)), 0.5, 2.0)
    up_scale = jnp.clip(jnp.exp(math.log(2.0) - 1.3862944 * jax.random.uniform(splits[5], (LAYERS, FF), jnp.float32) ** shard_levels(splits[5], (LAYERS, FF), ((1, 4),), -0.2, 0.2)), 0.5, 2.0)
    down_scale = jnp.clip(jnp.exp(math.log(2.0) - 1.3862944 * jax.random.uniform(splits[6], (LAYERS, D), jnp.float32) ** shard_levels(splits[6], (LAYERS, D), ((1, 4),), -0.2, 0.2)), 0.5, 2.0)
    pre_gain = jnp.clip(1.0 + 0.18 * jax.random.normal(splits[7], (LAYERS, D), jnp.float32), 0.1, 1.9)
    out_gain = jnp.clip(1.0 + 0.18 * jax.random.normal(splits[8], (D,), jnp.float32), 0.1, 1.9)
    return dict(stream=stream, w_gate=w_gate, w_up=w_up, w_down=w_down, gate_scale=gate_scale, up_scale=up_scale, down_scale=down_scale, pre_gain=pre_gain, out_gain=out_gain)


def reference(stream, w_gate, w_up, w_down, gate_scale, up_scale, down_scale, pre_gain, out_gain):
    current = stream
    for layer in range(LAYERS):
        xvals = lax.optimization_barrier(current).astype(jnp.float32)
        rinv = lax.rsqrt(lax.optimization_barrier(jnp.mean(xvals * xvals, axis=1, keepdims=True)) + 1e-06)
        scaled = (xvals * pre_gain[layer]).astype(jnp.bfloat16)
        gate = jnp.dot(scaled, w_gate[layer].astype(jnp.bfloat16), preferred_element_type=jnp.float32) * rinv * gate_scale[layer]
        upper = jnp.dot(scaled, w_up[layer].astype(jnp.bfloat16), preferred_element_type=jnp.float32) * rinv * up_scale[layer]
        hidden = (jax.nn.silu(gate) * upper).astype(jnp.bfloat16)
        blocks = hidden.astype(jnp.float32).reshape(TOK, N_CB, FF // N_CB)
        down_blocks = w_down[layer].astype(jnp.bfloat16).astype(jnp.float32).reshape(N_CB, FF // N_CB, D)
        partial_value = jnp.einsum('tcf,cfd->ctd', blocks, down_blocks).astype(jnp.bfloat16)
        branch = lax.optimization_barrier(jnp.sum(partial_value.astype(jnp.float32), axis=0)) * down_scale[layer]
        current = (0.5 * xvals + branch).astype(jnp.bfloat16)
    xvals = lax.optimization_barrier(current).astype(jnp.float32)
    rinv = lax.rsqrt(lax.optimization_barrier(jnp.mean(xvals * xvals, axis=1, keepdims=True)) + 1e-06)
    return (xvals * rinv * out_gain).astype(jnp.bfloat16)
```

```python
import functools

import jax
import jax.numpy as jnp
from jax import lax
from jax.experimental import pallas as pl
from jax.experimental.pallas import tpu as pltpu
from jax.sharding import PartitionSpec as P

F32, BF16 = jnp.float32, jnp.bfloat16
MESH = pl.DeviceIdType.MESH
EPS = 1e-06
WIDTH = 256
LAG = 2
PIECES = 4
UP_SLOTS = 6
DOWN_SLOTS = 12


def body(n, layers, dim, share, chunks, stream, wg, wu, wd, gs, us, ds, pg, og, out,
         wub, wdb, usem, dsem, xb, scaled, own, sr, sl, rr, rl, hid, acc, rinv_ref, ss,
         c1s, c1r, c2s, c2r, ssr, rsr, ssl, rsl, shr, shl, rh, sss, rss, cs, cr):
    p = lax.axis_index("ra")
    q = lax.axis_index("cb")
    core = lax.rem(q, 2)
    mate = q + 1 - 2 * core
    xmate = lax.rem(q + 2, 4)
    tokens, cols = stream.shape
    half = tokens // 2
    wide = cols // PIECES
    w = WIDTH
    total = layers * chunks

    def up_copies(t):
        l, c, k = t // chunks, lax.rem(t, chunks), lax.rem(t, UP_SLOTS)
        at = pl.ds(pl.multiple_of(c * w, w), w)
        return (pltpu.make_async_copy(wg.at[l, :, at], wub.at[k, 0], usem.at[k, 0]),
                pltpu.make_async_copy(wu.at[l, :, at], wub.at[k, 1], usem.at[k, 1]))

    def down_copy(t):
        l, c, k = t // chunks, lax.rem(t, chunks), lax.rem(t, DOWN_SLOTS)
        at = pl.ds(pl.multiple_of(c * w, w), w)
        return pltpu.make_async_copy(wd.at[l, at, :], wdb.at[k], dsem.at[k])

    @pl.loop(0, min(UP_SLOTS, total))
    def _(t):
        for copy in up_copies(t):
            copy.start()

    @pl.loop(0, min(DOWN_SLOTS, total))
    def _(t):
        down_copy(t).start()

    barrier = pltpu.get_barrier_semaphore()
    for k in range(1, n):
        pl.semaphore_signal(barrier, inc=1, device_id={"ra": lax.rem(p + k, n)}, device_id_type=MESH)
    pl.semaphore_signal(barrier, inc=1, device_id={"cb": mate}, device_id_type=MESH)
    pl.semaphore_signal(barrier, inc=1, device_id={"cb": xmate}, device_id_type=MESH)
    pl.semaphore_wait(barrier, n + 1)

    def remote(src, dst, send, recv, **where):
        return pltpu.make_async_remote_copy(src_ref=src, dst_ref=dst, send_sem=send, recv_sem=recv,
                                            device_id=where, device_id_type=MESH)

    right, left = jnp.minimum(p + 1, n - 1), jnp.maximum(p - 1, 0)

    def right_sum(t, c, d):
        return remote(sr.at[t, d], rr.at[t, d], ssr.at[c, d], rsr.at[c, d], ra=right)

    def left_sum(t, c, d):
        return remote(sl.at[t, d], rl.at[t, d], ssl.at[c, d], rsl.at[c, d], ra=left)

    def right_hid(t, c, o):
        return remote(hid.at[t, o], hid.at[t, o], shr.at[c, o], rh.at[c, o], ra=right)

    def left_hid(t, c, o):
        return remote(hid.at[t, o], hid.at[t, o], shl.at[c, o], rh.at[c, o], ra=left)

    def square_copy(l, k, src):
        return remote(ss.at[l, src], ss.at[l, src], sss.at[l, k], rss.at[l, src], ra=lax.rem(p + k, n))

    def send_squares(l):
        col = jnp.zeros((tokens, 1), F32)
        for j in range(PIECES):
            x = xb[l, j].astype(F32)
            col += jnp.sum(x * x, axis=1, keepdims=True)
        eye = (lax.broadcasted_iota(jnp.int32, (tokens, tokens), 0)
               == lax.broadcasted_iota(jnp.int32, (tokens, tokens), 1))
        row = jnp.sum(jnp.where(eye, col, 0.0), axis=0, keepdims=True)
        ss[l, p] = jnp.broadcast_to(row, (8, tokens))
        for k in range(1, n):
            square_copy(l, k, p).start()

    def take_rinv(l, first, rows):
        for k in range(1, n):
            src = lax.rem(p + k, n)
            square_copy(l, k, src).wait_recv()
        row = ss[l, 0][0:1]
        for src in range(1, n):
            row = row + ss[l, src][0:1]
        pick = (lax.broadcasted_iota(jnp.int32, (rows, tokens), 0) + first
                == lax.broadcasted_iota(jnp.int32, (rows, tokens), 1))
        col = jnp.sum(jnp.where(pick, row, 0.0), axis=1, keepdims=True)
        return lax.rsqrt(col / dim + EPS)

    def end_squares(l):
        for k in range(1, n):
            square_copy(l, k, p).wait_send()

    for j in range(PIECES):
        xb[0, j] = stream[:, j * wide:(j + 1) * wide]

    def layer(l):
        send_squares(l)
        for j in range(PIECES):
            at = pl.ds(j * wide, wide)
            scaled[:, at] = (xb[l, j].astype(F32) * pg[pl.ds(l, 1), at]).astype(BF16)
        acc[...] = jnp.zeros_like(acc)

        def products(c):
            t = l * chunks + c
            k = lax.rem(t, UP_SLOTS)
            for copy in up_copies(t):
                copy.wait()
            for side in range(2):
                part = jnp.dot(scaled[...], wub[k, side].astype(BF16), preferred_element_type=F32)
                for d in range(n):
                    own[c, d, :, side * w:(side + 1) * w] = part[d * share:(d + 1) * share]

            @pl.when(t + UP_SLOTS < total)
            def _():
                for copy in up_copies(t + UP_SLOTS):
                    copy.start()

            @pl.when(p == 0)
            def _():
                for d in range(n - 1, 0, -1):
                    sr[t, d] = own[c, d].astype(BF16)
                    right_sum(t, c, d).start()

            @pl.when(p == n - 1)
            def _():
                for d in range(n - 1):
                    sl[t, d] = own[c, d].astype(BF16)
                    left_sum(t, c, d).start()

        def hop(c, h):
            t = l * chunks + c

            @pl.when(p == h)
            def _():
                for d in range(n - 1, h, -1):
                    right_sum(t, c, d).wait_recv()
                    sr[t, d] = (own[c, d] + rr[t, d].astype(F32)).astype(BF16)
                    right_sum(t, c, d).start()

            @pl.when(p == n - 1 - h)
            def _():
                for d in range(n - 1 - h):
                    left_sum(t, c, d).wait_recv()
                    sl[t, d] = (own[c, d] + rl[t, d].astype(F32)).astype(BF16)
                    left_sum(t, c, d).start()

        def finish(c):
            t = l * chunks + c

            @pl.when(c == 0)
            def _():
                rinv_ref[...] = jnp.broadcast_to(take_rinv(l, p * share, share), rinv_ref.shape)

            @pl.when(p > 0)
            def _():
                right_sum(t, c, p).wait_recv()
                own[c, p] += rr[t, p].astype(F32)

            @pl.when(p < n - 1)
            def _():
                left_sum(t, c, p).wait_recv()
                own[c, p] += rl[t, p].astype(F32)

            at = pl.ds(pl.multiple_of(c * w, w), w)
            rinv = rinv_ref[:, 0:1]
            gate = own[c, p, :, 0:w] * rinv * gs[pl.ds(l, 1), at]
            upper = own[c, p, :, w:2 * w] * rinv * us[pl.ds(l, 1), at]
            hid[t, p] = (gate / (1.0 + jnp.exp(-gate)) * upper).astype(BF16)

            @pl.when(p < n - 1)
            def _():
                right_hid(t, c, p).start()

            @pl.when(p > 0)
            def _():
                left_hid(t, c, p).start()

        def pass_on(c, k):
            t = l * chunks + c

            @pl.when(p >= k)
            def _():
                right_hid(t, c, p - k).wait_recv()

                @pl.when(p < n - 1)
                def _():
                    right_hid(t, c, p - k).start()

            @pl.when(p + k <= n - 1)
            def _():
                left_hid(t, c, p + k).wait_recv()

                @pl.when(p > 0)
                def _():
                    left_hid(t, c, p + k).start()

        def down(c):
            t = l * chunks + c
            k = lax.rem(t, DOWN_SLOTS)
            down_copy(t).wait()
            rows = jnp.concatenate([hid[t, d] for d in range(n)], axis=0)
            acc[...] += jnp.dot(rows, wdb[k].astype(BF16), preferred_element_type=F32)

            @pl.when(t + DOWN_SLOTS < total)
            def _():
                down_copy(t + DOWN_SLOTS).start()

        stages = [products]
        stages += [functools.partial(hop, h=h) for h in range(1, n - 1)]
        stages += [finish]
        stages += [functools.partial(pass_on, k=k) for k in range(1, n)]

        @pl.loop(0, chunks + LAG * (len(stages) - 1))
        def _(i):
            for place, stage in enumerate(stages):
                c = i - LAG * place

                @pl.when((c >= 0) & (c < chunks))
                def _(stage=stage, c=c):
                    stage(c)
                    if place == len(stages) - 1:
                        down(c)

        def core_copy(j):
            return remote(c1s.at[l, j], c1r.at[l, j], cs.at[0, l, j], cr.at[0, l, j], cb=mate)

        def chip_copy(j):
            return remote(c2s.at[l, j], c2r.at[l, j], cs.at[1, l, j], cr.at[1, l, j], cb=xmate)

        mine = pl.ds(pl.multiple_of(core * half, half), half)
        other = pl.ds(pl.multiple_of((1 - core) * half, half), half)

        def back_copy(j, rows):
            return remote(xb.at[l + 1, j, rows], xb.at[l + 1, j, rows],
                          cs.at[2, l, j], cr.at[2, l, j], cb=mate)

        for j in range(PIECES):
            c1s[l, j] = acc[other, j * wide:(j + 1) * wide].astype(BF16)
            core_copy(j).start()
        for j in range(PIECES):
            core_copy(j).wait_recv()
            c2s[l, j] = (acc[mine, j * wide:(j + 1) * wide] + c1r[l, j].astype(F32)).astype(BF16)
            chip_copy(j).start()

        @pl.loop(0, chunks)
        def _(c):
            t = l * chunks + c
            for d in range(n):
                @pl.when(p < d)
                def _():
                    right_sum(t, c, d).wait_send()

                @pl.when(p > d)
                def _():
                    left_sum(t, c, d).wait_send()

                @pl.when((d <= p) & (p < n - 1))
                def _():
                    right_hid(t, c, d).wait_send()

                @pl.when((d >= p) & (p > 0))
                def _():
                    left_hid(t, c, d).wait_send()
        end_squares(l)

        for j in range(PIECES):
            chip_copy(j).wait_recv()
            at = pl.ds(j * wide, wide)
            branch = (c2s[l, j].astype(F32) + c2r[l, j].astype(F32)) * ds[pl.ds(l, 1), at]
            xb[l + 1, j, mine] = (0.5 * xb[l, j, mine].astype(F32) + branch).astype(BF16)
            back_copy(j, mine).start()
        for j in range(PIECES):
            back_copy(j, other).wait_recv()
            core_copy(j).wait_send()
            chip_copy(j).wait_send()
            back_copy(j, mine).wait_send()

    pl.loop(0, layers)(layer)

    send_squares(layers)
    rinv = take_rinv(layers, 0, tokens)
    for j in range(PIECES):
        at = slice(j * wide, (j + 1) * wide)
        out[:, at] = (xb[layers, j].astype(F32) * rinv * og[0:1, at]).astype(BF16)
    end_squares(layers)


def fused(stream, w_gate, w_up, w_down, gate_scale, up_scale, down_scale, pre_gain, out_gain):
    n = lax.axis_size("ra")
    tokens, cols = stream.shape
    layers, _, units = w_gate.shape
    share, chunks, half, wide = tokens // n, units // WIDTH, tokens // 2, cols // PIECES
    total = layers * chunks
    dma = pltpu.SemaphoreType.DMA
    scratch = [
        pltpu.VMEM((UP_SLOTS, 2, cols, WIDTH), F32),
        pltpu.VMEM((DOWN_SLOTS, WIDTH, cols), F32),
        dma((UP_SLOTS, 2)),
        dma((DOWN_SLOTS,)),
        pltpu.VMEM((layers + 1, PIECES, tokens, wide), BF16),
        pltpu.VMEM((tokens, cols), BF16),
        pltpu.VMEM((chunks, n, share, 2 * WIDTH), F32),
        pltpu.VMEM((total, n, share, 2 * WIDTH), BF16),
        pltpu.VMEM((total, n, share, 2 * WIDTH), BF16),
        pltpu.VMEM((total, n, share, 2 * WIDTH), BF16),
        pltpu.VMEM((total, n, share, 2 * WIDTH), BF16),
        pltpu.VMEM((total, n, share, WIDTH), BF16),
        pltpu.VMEM((tokens, cols), F32),
        pltpu.VMEM((share, 128), F32),
        pltpu.VMEM((layers + 1, n, 8, tokens), F32),
    ]
    scratch += [pltpu.VMEM((layers, PIECES, half, wide), BF16)] * 4
    scratch += [dma((chunks, n))] * 7
    scratch += [dma((layers + 1, n))] * 2
    scratch += [dma((3, layers, PIECES))] * 2
    vmem, hbm = pl.BlockSpec(memory_space=pltpu.VMEM), pl.BlockSpec(memory_space=pl.ANY)
    return pl.pallas_call(
        functools.partial(body, n, layers, cols * n, share, chunks),
        out_shape=jax.ShapeDtypeStruct((tokens, cols), BF16),
        in_specs=[vmem, hbm, hbm, hbm] + [vmem] * 5,
        out_specs=vmem,
        scratch_shapes=scratch,
        compiler_params=pltpu.CompilerParams(
            collective_id=0, has_side_effects=True, vmem_limit_bytes=64 * 1024 * 1024 - 65536
        ),
    )(stream, w_gate, w_up, w_down, gate_scale, up_scale, down_scale, pre_gain, out_gain[None])


def plain(stream, w_gate, w_up, w_down, gate_scale, up_scale, down_scale, pre_gain, out_gain):
    current = stream
    tokens = stream.shape[0]
    dim = stream.shape[1] * lax.axis_size("ra")
    share = tokens // lax.axis_size("ra")
    for layer in range(w_gate.shape[0]):
        xvals = current.astype(F32)
        squares = jnp.sum(xvals * xvals, axis=1)
        scaled = (xvals * pre_gain[layer]).astype(BF16)
        gate_part = jnp.dot(scaled, w_gate[layer].astype(BF16), preferred_element_type=F32)
        up_part = jnp.dot(scaled, w_up[layer].astype(BF16), preferred_element_type=F32)
        down_local = w_down[layer].astype(BF16)
        total = lax.psum(squares, "ra")
        summed = (
            lax.psum_scatter(gate_part, "ra", scatter_dimension=0, tiled=True),
            lax.psum_scatter(up_part, "ra", scatter_dimension=0, tiled=True),
        )
        own_rows = lax.dynamic_slice_in_dim(total, lax.axis_index("ra") * share, share)
        rinv = lax.rsqrt(own_rows / dim + EPS)[:, None]
        gate = summed[0] * rinv * gate_scale[layer]
        upper = summed[1] * rinv * up_scale[layer]
        hidden = (jax.nn.silu(gate) * upper).astype(BF16)
        terms = jnp.dot(
            lax.all_gather(hidden, "ra", axis=0, tiled=True), down_local, preferred_element_type=F32
        )
        branch = lax.psum(terms.astype(BF16), "cb").astype(F32) * down_scale[layer]
        current = (0.5 * xvals + branch).astype(BF16)
    xvals = current.astype(F32)
    final_sum = lax.psum(jnp.sum(xvals * xvals, axis=1), "ra")
    rinv = lax.rsqrt(final_sum / dim + EPS)[:, None]
    return (xvals * rinv * out_gain).astype(BF16)


def local(*args):
    n = lax.axis_size("ra")
    tokens, cols = args[0].shape
    fits = (n >= 2 and tokens % (16 * n) == 0 and tokens == 128 and lax.axis_size("cb") == 4
            and args[1].shape[2] % WIDTH == 0 and cols % (128 * PIECES) == 0)
    return (fused if fits else plain)(*args)


def solution(mesh):
    placed = (
        P("grp", "ra"),
        P(None, "ra", "cb"),
        P(None, "ra", "cb"),
        P(None, "cb", "ra"),
        P(None, "cb"),
        P(None, "cb"),
        P(None, "ra"),
        P(None, "ra"),
        P("ra"),
    )
    return jax.shard_map(
        local, mesh=mesh, in_specs=placed, out_specs=P("grp", "ra"), check_vma=False
    )
```

```python
import functools

import jax
import jax.numpy as jnp
from jax import lax
from jax.experimental import pallas as pl
from jax.experimental.pallas import tpu as pltpu
from jax.sharding import PartitionSpec as P

F32, BF16 = jnp.float32, jnp.bfloat16
MESH = pl.DeviceIdType.MESH
EPS = 1e-06
WIDTH = 256
LAG = 3
PIECES = 2
UP_SLOTS = 6
FIRST = 2
DOWN_SLOTS = 12


def body(n, layers, dim, share, chunks, stream, wg, wu, wd, gs, us, ds, pg, og, out,
         wub, wdb, usem, dsem, xb, scaled, own, sums, got, hid, acc, rinv_ref, scales, ss,
         c1s, c1r, c2s, c2r, ssum, rsum, shid, rhid, sss, rss, cs, cr):
    p = lax.axis_index("ra")
    q = lax.axis_index("cb")
    core = lax.rem(q, 2)
    mate = q + 1 - 2 * core
    xmate = lax.rem(q + 2, 4)
    tokens, cols = stream.shape
    half = tokens // 2
    wide = cols // PIECES
    w = WIDTH
    total = layers * chunks

    def up_copies(t):
        l, c, k = t // chunks, lax.rem(t, chunks), lax.rem(t, UP_SLOTS)
        at = pl.ds(pl.multiple_of(c * w, w), w)
        return (pltpu.make_async_copy(wg.at[l, :, at], wub.at[k, 0], usem.at[k, 0]),
                pltpu.make_async_copy(wu.at[l, :, at], wub.at[k, 1], usem.at[k, 1]))

    def down_copy(t):
        l, c, k = t // chunks, lax.rem(t, chunks), lax.rem(t, DOWN_SLOTS)
        at = pl.ds(pl.multiple_of(c * w, w), w)
        return pltpu.make_async_copy(wd.at[l, at, :], wdb.at[k], dsem.at[k])

    for t in range(FIRST):
        for copy in up_copies(t):
            copy.start()

    barrier = pltpu.get_barrier_semaphore()
    for k in range(1, n):
        pl.semaphore_signal(barrier, inc=1, device_id={"ra": lax.rem(p + k, n)}, device_id_type=MESH)
    pl.semaphore_signal(barrier, inc=1, device_id={"cb": mate}, device_id_type=MESH)
    pl.semaphore_signal(barrier, inc=1, device_id={"cb": xmate}, device_id_type=MESH)
    pl.semaphore_wait(barrier, n + 1)

    def remote(src, dst, send, recv, **where):
        return pltpu.make_async_remote_copy(src_ref=src, dst_ref=dst, send_sem=send, recv_sem=recv,
                                            device_id=where, device_id_type=MESH)

    right, left = jnp.minimum(p + 1, n - 1), jnp.maximum(p - 1, 0)

    def sum_copy(t, c, e):
        return remote(sums.at[t, e], got.at[t, e], ssum.at[c, e], rsum.at[c, e], ra=right if e else left)

    def hid_copy(t, c, e):
        return remote(hid.at[t, e], hid.at[t, e], shid.at[c, e], rhid.at[c, e], ra=left if e else right)

    def square_copy(l, k, src):
        return remote(ss.at[l, src], ss.at[l, src], sss.at[l, k], rss.at[l, src], ra=lax.rem(p + k, n))

    def send_squares(l):
        col = jnp.zeros((tokens, 1), F32)
        for j in range(PIECES):
            x = xb[l, j].astype(F32)
            col += jnp.sum(x * x, axis=1, keepdims=True)
        eye = (lax.broadcasted_iota(jnp.int32, (tokens, tokens), 0)
               == lax.broadcasted_iota(jnp.int32, (tokens, tokens), 1))
        row = jnp.sum(jnp.where(eye, col, 0.0), axis=0, keepdims=True)
        ss[l, p] = jnp.broadcast_to(row, (8, tokens))
        for k in range(1, n):
            square_copy(l, k, p).start()

    def take_rinv(l, first, rows):
        for k in range(1, n):
            src = lax.rem(p + k, n)
            square_copy(l, k, src).wait_recv()
        row = ss[l, 0][0:1]
        for src in range(1, n):
            row = row + ss[l, src][0:1]
        pick = (lax.broadcasted_iota(jnp.int32, (rows, tokens), 0) + first
                == lax.broadcasted_iota(jnp.int32, (rows, tokens), 1))
        col = jnp.sum(jnp.where(pick, row, 0.0), axis=1, keepdims=True)
        return lax.rsqrt(col / dim + EPS)

    def end_squares(l):
        for k in range(1, n):
            square_copy(l, k, p).wait_send()

    for t in range(total):
        row, at = slice(t // chunks, t // chunks + 1), slice(t % chunks * w, (t % chunks + 1) * w)
        scales[t, 0:1] = gs[row, at]
        scales[t, 1:2] = us[row, at]
    for j in range(PIECES):
        xb[0, j] = stream[:, j * wide:(j + 1) * wide]

    def layer(l):
        send_squares(l)
        for j in range(PIECES):
            at = pl.ds(j * wide, wide)
            scaled[:, at] = (xb[l, j].astype(F32) * pg[pl.ds(l, 1), at]).astype(BF16)
        acc[...] = jnp.zeros_like(acc)

        def products(c):
            t = l * chunks + c
            k = lax.rem(t, UP_SLOTS)
            for copy in up_copies(t):
                copy.wait()

            @pl.when(t == 0)
            def _():
                @pl.loop(FIRST, min(UP_SLOTS, total))
                def _(later):
                    for copy in up_copies(later):
                        copy.start()

                @pl.loop(0, min(DOWN_SLOTS, total))
                def _(later):
                    down_copy(later).start()

            for side in range(2):
                part = jnp.dot(scaled[...], wub[k, side].astype(BF16), preferred_element_type=F32)
                for e in range(2):
                    own[c, e, :, side * w:(side + 1) * w] = part[e * share:(e + 1) * share]

            @pl.when(t + UP_SLOTS < total)
            def _():
                for copy in up_copies(t + UP_SLOTS):
                    copy.start()

            for e in range(2):
                @pl.when(p == (0 if e else n - 1))
                def _():
                    sums[t, e] = own[c, e].astype(BF16)
                    sum_copy(t, c, e).start()

        def hop(c, h):
            t = l * chunks + c
            for e in range(2):
                @pl.when(p == (h if e else n - 1 - h))
                def _():
                    sum_copy(t, c, e).wait_recv()
                    sums[t, e] = (own[c, e] + got[t, e].astype(F32)).astype(BF16)
                    sum_copy(t, c, e).start()

        def finish(c):
            @pl.when(c == 0)
            def _():
                first = jnp.where(p == 0, 0, share)
                rinv_ref[...] = jnp.broadcast_to(take_rinv(l, first, share), rinv_ref.shape)

            for e in range(2):
                @pl.when(p == (n - 1 if e else 0))
                def _():
                    activate(c, e)

        def activate(c, e):
            t = l * chunks + c
            sum_copy(t, c, e).wait_recv()
            both = own[c, e] + got[t, e].astype(F32)
            rinv = rinv_ref[:, 0:1]
            gate = both[:, 0:w] * rinv * scales[t, 0:1]
            upper = both[:, w:2 * w] * rinv * scales[t, 1:2]
            hid[t, e] = (gate / (1.0 + jnp.exp(-gate)) * upper).astype(BF16)
            hid_copy(t, c, e).start()

        def pass_on(c, k):
            t = l * chunks + c
            for e in range(2):
                @pl.when(p == (n - 1 - k if e else k))
                def _():
                    hid_copy(t, c, e).wait_recv()
                    if k < n - 1:
                        hid_copy(t, c, e).start()

        def down(c):
            t = l * chunks + c
            k = lax.rem(t, DOWN_SLOTS)
            down_copy(t).wait()
            rows = jnp.concatenate([hid[t, 0], hid[t, 1]], axis=0)
            acc[...] += jnp.dot(rows, wdb[k].astype(BF16), preferred_element_type=F32)

            @pl.when(t + DOWN_SLOTS < total)
            def _():
                down_copy(t + DOWN_SLOTS).start()

        stages = [products]
        stages += [functools.partial(hop, h=h) for h in range(1, n - 1)]
        stages += [finish]
        stages += [functools.partial(pass_on, k=k) for k in range(1, n)]

        @pl.loop(0, chunks + LAG * (len(stages) - 1))
        def _(i):
            for place, stage in enumerate(stages):
                c = i - LAG * place

                @pl.when((c >= 0) & (c < chunks))
                def _(stage=stage, c=c):
                    stage(c)
                    if place == len(stages) - 1:
                        down(c)

        def core_copy(j):
            return remote(c1s.at[l, j], c1r.at[l, j], cs.at[0, l, j], cr.at[0, l, j], cb=mate)

        def chip_copy(j):
            return remote(c2s.at[l, j], c2r.at[l, j], cs.at[1, l, j], cr.at[1, l, j], cb=xmate)

        mine = pl.ds(pl.multiple_of(core * half, half), half)
        other = pl.ds(pl.multiple_of((1 - core) * half, half), half)

        def back_copy(j, rows):
            return remote(xb.at[l + 1, j, rows], xb.at[l + 1, j, rows],
                          cs.at[2, l, j], cr.at[2, l, j], cb=mate)

        for j in range(PIECES):
            c1s[l, j] = acc[other, j * wide:(j + 1) * wide].astype(BF16)
            core_copy(j).start()
        for j in range(PIECES):
            core_copy(j).wait_recv()
            c2s[l, j] = (acc[mine, j * wide:(j + 1) * wide] + c1r[l, j].astype(F32)).astype(BF16)
            chip_copy(j).start()

        @pl.loop(0, chunks)
        def _(c):
            t = l * chunks + c
            for e in range(2):
                @pl.when(p != (n - 1 if e else 0))
                def _():
                    sum_copy(t, c, e).wait_send()

                @pl.when(p != (0 if e else n - 1))
                def _():
                    hid_copy(t, c, e).wait_send()
        end_squares(l)

        for j in range(PIECES):
            chip_copy(j).wait_recv()
            at = pl.ds(j * wide, wide)
            branch = (c2s[l, j].astype(F32) + c2r[l, j].astype(F32)) * ds[pl.ds(l, 1), at]
            xb[l + 1, j, mine] = (0.5 * xb[l, j, mine].astype(F32) + branch).astype(BF16)
            back_copy(j, mine).start()
        for j in range(PIECES):
            back_copy(j, other).wait_recv()
            core_copy(j).wait_send()
            chip_copy(j).wait_send()
            back_copy(j, mine).wait_send()

    pl.loop(0, layers)(layer)

    send_squares(layers)
    rinv = take_rinv(layers, 0, tokens)
    for j in range(PIECES):
        at = slice(j * wide, (j + 1) * wide)
        out[:, at] = (xb[layers, j].astype(F32) * rinv * og[0:1, at]).astype(BF16)
    end_squares(layers)


def fused(stream, w_gate, w_up, w_down, gate_scale, up_scale, down_scale, pre_gain, out_gain):
    n = lax.axis_size("ra")
    tokens, cols = stream.shape
    layers, _, units = w_gate.shape
    share, chunks, half, wide = tokens // 2, units // WIDTH, tokens // 2, cols // PIECES
    total = layers * chunks
    dma = pltpu.SemaphoreType.DMA
    scratch = [
        pltpu.VMEM((UP_SLOTS, 2, cols, WIDTH), F32),
        pltpu.VMEM((DOWN_SLOTS, WIDTH, cols), F32),
        dma((UP_SLOTS, 2)),
        dma((DOWN_SLOTS,)),
        pltpu.VMEM((layers + 1, PIECES, tokens, wide), BF16),
        pltpu.VMEM((tokens, cols), BF16),
        pltpu.VMEM((chunks, 2, share, 2 * WIDTH), F32),
        pltpu.VMEM((total, 2, share, 2 * WIDTH), BF16),
        pltpu.VMEM((total, 2, share, 2 * WIDTH), BF16),
        pltpu.VMEM((total, 2, share, WIDTH), BF16),
        pltpu.VMEM((tokens, cols), F32),
        pltpu.VMEM((share, 128), F32),
        pltpu.VMEM((total, 8, WIDTH), F32),
        pltpu.VMEM((layers + 1, n, 8, tokens), F32),
    ]
    scratch += [pltpu.VMEM((layers, PIECES, half, wide), BF16)] * 4
    scratch += [dma((chunks, 2))] * 4
    scratch += [dma((layers + 1, n))] * 2
    scratch += [dma((3, layers, PIECES))] * 2
    vmem, hbm = pl.BlockSpec(memory_space=pltpu.VMEM), pl.BlockSpec(memory_space=pl.ANY)
    return pl.pallas_call(
        functools.partial(body, n, layers, cols * n, share, chunks),
        out_shape=jax.ShapeDtypeStruct((tokens, cols), BF16),
        in_specs=[vmem, hbm, hbm, hbm] + [vmem] * 5,
        out_specs=vmem,
        scratch_shapes=scratch,
        compiler_params=pltpu.CompilerParams(
            collective_id=0, has_side_effects=True, vmem_limit_bytes=64 * 1024 * 1024 - 65536
        ),
    )(stream, w_gate, w_up, w_down, gate_scale, up_scale, down_scale, pre_gain, out_gain[None])


def plain(stream, w_gate, w_up, w_down, gate_scale, up_scale, down_scale, pre_gain, out_gain):
    current = stream
    tokens = stream.shape[0]
    dim = stream.shape[1] * lax.axis_size("ra")
    share = tokens // lax.axis_size("ra")
    for layer in range(w_gate.shape[0]):
        xvals = current.astype(F32)
        squares = jnp.sum(xvals * xvals, axis=1)
        scaled = (xvals * pre_gain[layer]).astype(BF16)
        gate_part = jnp.dot(scaled, w_gate[layer].astype(BF16), preferred_element_type=F32)
        up_part = jnp.dot(scaled, w_up[layer].astype(BF16), preferred_element_type=F32)
        down_local = w_down[layer].astype(BF16)
        total = lax.psum(squares, "ra")
        summed = (
            lax.psum_scatter(gate_part, "ra", scatter_dimension=0, tiled=True),
            lax.psum_scatter(up_part, "ra", scatter_dimension=0, tiled=True),
        )
        own_rows = lax.dynamic_slice_in_dim(total, lax.axis_index("ra") * share, share)
        rinv = lax.rsqrt(own_rows / dim + EPS)[:, None]
        gate = summed[0] * rinv * gate_scale[layer]
        upper = summed[1] * rinv * up_scale[layer]
        hidden = (jax.nn.silu(gate) * upper).astype(BF16)
        terms = jnp.dot(
            lax.all_gather(hidden, "ra", axis=0, tiled=True), down_local, preferred_element_type=F32
        )
        branch = lax.psum(terms.astype(BF16), "cb").astype(F32) * down_scale[layer]
        current = (0.5 * xvals + branch).astype(BF16)
    xvals = current.astype(F32)
    final_sum = lax.psum(jnp.sum(xvals * xvals, axis=1), "ra")
    rinv = lax.rsqrt(final_sum / dim + EPS)[:, None]
    return (xvals * rinv * out_gain).astype(BF16)


def local(*args):
    n = lax.axis_size("ra")
    tokens, cols = args[0].shape
    fits = (n >= 2 and tokens == 128 and n <= 8 and lax.axis_size("cb") == 4
            and args[1].shape[2] % WIDTH == 0 and cols % (128 * PIECES) == 0)
    return (fused if fits else plain)(*args)


def solution(mesh):
    placed = (
        P("grp", "ra"),
        P(None, "ra", "cb"),
        P(None, "ra", "cb"),
        P(None, "cb", "ra"),
        P(None, "cb"),
        P(None, "cb"),
        P(None, "ra"),
        P(None, "ra"),
        P("ra"),
    )
    return jax.shard_map(
        local, mesh=mesh, in_specs=placed, out_specs=P("grp", "ra"), check_vma=False
    )
```
